32 devices in a mesh: fs: 8 (over z, x), tp: 4 (over y, core).
Axes of the slice: x: 2, y: 2, z: 4, core: 2. Of those that a mesh axis runs over, the one named last changes fastest.
Arguments:
- tokens: bfloat16 [4096, 2048], P(('fs', 'tp')), may hold values from -6 to 6
- gate_weight: bfloat16 [2048, 6144], P('fs', 'tp'), may hold values from -0.125 to 0.125
- value_weight: bfloat16 [2048, 6144], P('fs', 'tp'), may hold values from -0.125 to 0.125
- gate_taps: float32 [3, 6144], P(None, 'tp'), may hold values from -3.5 to 3.5
- value_taps: float32 [3, 6144], P(None, 'tp'), may hold values from -3.5 to 3.5
- down_weight: bfloat16 [6144, 2048], P('tp', 'fs'), may hold values from -0.078125 to 0.078125
- norm_gain: float32 [2048], replicated, may hold values from 0.1 to 1.9
- norm_shift: float32 [2048], replicated, may hold values from -3 to 3
Outputs:
- mixed: bfloat16 [4096, 2048], P(('fs', 'tp'))
The draws below stay inside these ranges and needn't reach their ends.
All inputs are finite; a program needn't handle non-finite values.
Results may differ from the reference program's by a relative error of at most 0.017.
Values may be sent and summed in bfloat16 or wider, within the bound.
A program may use at most 256 MiB of HBM per device.

```python
import jax
import jax.numpy as jnp
from jax import lax

D = 2048
FF = 6144
TAPS = 3
TOK_DEV = 128
TOKENS = 4096
N_FS = 8
N_TP = 4


def block_scale(own_key, shape, cuts, smallest, top_value):
    level = 1.0
    for position, blocks in cuts:
        draws = jax.random.uniform(jax.random.fold_in(jax.random.fold_in(own_key, 6), position), (blocks,), jnp.float32, smallest / len(cuts), top_value / len(cuts))
        level = level * jnp.repeat(jnp.exp(draws), shape[position] // blocks).reshape((-1,) + (1,) * (len(shape) - 1 - position))
    return level


def bell_draw(stream_key, shape, width, reach, shards=(), dtype=jnp.bfloat16):
    array = width * jax.random.normal(stream_key, shape, jnp.float32)
    if shards:
        array = array * block_scale(stream_key, shape, shards, -0.22, 0.18)
    return jnp.clip(array, -reach, reach).astype(dtype)


def setup_inputs(seed: int = 0) -> dict:
    arg_keys = jax.random.split(jax.random.key(seed), 9)
    tokens = bell_draw(arg_keys[0], (TOKENS, D), 1.0, 6.0, ((0, 32),))
    gate_weight = bell_draw(arg_keys[1], (D, FF), D ** -0.5, 0.125, ((0, 8), (1, 4)))
    value_weight = bell_draw(arg_keys[2], (D, FF), D ** -0.5, 0.125, ((0, 8), (1, 4)))
    gate_taps = bell_draw(arg_keys[3], (TAPS, FF), TAPS ** -0.5, 3.5, ((1, 4),), jnp.float32)
    value_taps = bell_draw(arg_keys[4], (TAPS, FF), TAPS ** -0.5, 3.5, ((1, 4),), jnp.float32)
    down_weight = bell_draw(arg_keys[5], (FF, D), FF ** -0.5, 0.078125, ((0, 4), (1, 8)))
    norm_gain = jnp.clip(1.0 + 0.18 * jax.random.normal(arg_keys[6], (D,), jnp.float32), 0.1, 1.9)
    norm_shift = bell_draw(arg_keys[7], (D,), 0.5, 3.0, (), jnp.float32)
    return dict(tokens=tokens, gate_weight=gate_weight, value_weight=value_weight, gate_taps=gate_taps, value_taps=value_taps, down_weight=down_weight, norm_gain=norm_gain, norm_shift=norm_shift)


def causal_mix(pre, kernel_taps):
    leading = jnp.zeros((2, pre.shape[1]), jnp.float32)
    padded = jnp.concatenate([leading, pre.astype(jnp.float32)], axis=0)
    length = pre.shape[0]
    return kernel_taps[0] * padded[0:length] + kernel_taps[1] * padded[1:length + 1] + kernel_taps[2] * padded[2:length + 2]

def one_sequence(rows, gate_weight, value_weight, gate_taps, value_taps, down_weight, norm_gain, norm_shift):
    gate_pre = jnp.dot(rows, gate_weight, preferred_element_type=jnp.float32).astype(jnp.bfloat16)
    value_pre = jnp.dot(rows, value_weight, preferred_element_type=jnp.float32).astype(jnp.bfloat16)
    gate_mix = causal_mix(gate_pre, gate_taps)
    value_mix = causal_mix(value_pre, value_taps)
    hidden = (jax.nn.gelu(gate_mix, approximate=False) * value_mix).astype(jnp.bfloat16)
    length = rows.shape[0]
    block_cols = FF // N_TP
    hidden_blocks = hidden.reshape(length, N_TP, block_cols).astype(jnp.float32)
    down_blocks = down_weight.reshape(N_TP, block_cols, D).astype(jnp.float32)
    partials = jnp.einsum('lkf,kfd->kld', hidden_blocks, down_blocks).astype(jnp.bfloat16)
    summed = lax.optimization_barrier(jnp.sum(partials.astype(jnp.float32), axis=0))
    average = lax.optimization_barrier(jnp.mean(summed, axis=1, keepdims=True))
    centered = summed - average
    variance = lax.optimization_barrier(jnp.mean(centered * centered, axis=1, keepdims=True))
    normed = centered * lax.rsqrt(variance + 1e-05) * norm_gain + norm_shift
    return normed.astype(jnp.bfloat16)

def reference(tokens, gate_weight, value_weight, gate_taps, value_taps, down_weight, norm_gain, norm_shift):
    length = TOK_DEV * N_TP
    grouped = tokens.reshape(N_FS, length, D)
    result = lax.map(lambda rows: one_sequence(rows, gate_weight, value_weight, gate_taps, value_taps, down_weight, norm_gain, norm_shift), grouped)
    return result.reshape(N_FS * length, D)
```

```python
import functools

import jax
import jax.numpy as jnp
from jax import lax
from jax.experimental import pallas as pl
from jax.experimental.pallas import tpu as pltpu
from jax.sharding import PartitionSpec as P

MESH = pl.DeviceIdType.MESH
LEAD = 8


def kernel(
    dims,
    x_ref, g_ref, v_ref, gt_ref, vt_ref, d_ref, gain_ref, shift_ref,
    out_ref,
    tok, gw, vw, dw, pre_g, pre_v, part, rc, ry, zr,
    tok_r, tz_s, ty_s, tc_s, w_r, wz_s, wx_s, rc_r, rc_s, ry_r, ry_s, zc_r, zc_s,
):
    nz, nx, ny, nc = dims
    rows, width = x_ref.shape
    depth = g_ref.shape[0]
    units = gw.shape[1]
    cols = d_ref.shape[1]
    fs = lax.axis_index("fs")
    tp = lax.axis_index("tp")
    z, x = fs // nx, fs % nx
    y, c = tp // nc, tp % nc
    length = ny * nc * rows

    def at(zz=z, xx=x, yy=y, cc=c):
        return {"fs": zz * nx + xx, "tp": yy * nc + cc}

    z_others = [(z + i) % nz for i in range(1, nz)]
    x_others = [(x + i) % nx for i in range(1, nx)]
    y_others = [(y + i) % ny for i in range(1, ny)]
    c_others = [(c + i) % nc for i in range(1, nc)]

    barrier = pltpu.get_barrier_semaphore()
    partners = (
        [at(zz=i) for i in z_others]
        + [at(xx=i) for i in x_others]
        + [at(yy=i) for i in y_others]
        + [at(cc=i) for i in c_others]
    )
    for partner in partners:
        pl.semaphore_signal(barrier, inc=1, device_id=partner, device_id_type=MESH)
    pl.semaphore_wait(barrier, len(partners))

    def copy(src, dst, send, recv, device):
        return pltpu.make_async_remote_copy(
            src_ref=src, dst_ref=dst, send_sem=send, recv_sem=recv,
            device_id=device, device_id_type=MESH,
        )

    def slot(zz, t):
        return tok.at[zz, pl.ds(pl.multiple_of(t * rows, rows), rows)]

    def tok_copy(src, zz, t, send, device):
        return copy(src, slot(zz, t), send, tok_r.at[zz, t], device)

    def tok_z(src, zz, way):
        return tok_copy(src, zz, tp, tz_s.at[way, zz], at(zz=z + 1 - 2 * way))

    def tok_y(src, zz, yy):
        return tok_copy(src, zz, tp, ty_s.at[zz, yy], at(yy=yy))

    def tok_c(src, zz, yy, cc):
        return tok_copy(src, zz, yy * nc + c, tc_s.at[zz, yy, cc], at(cc=cc))

    def tok_wait(zz, t):
        tok_copy(slot(zz, t), zz, t, tz_s.at[0, 0], partners[0]).wait_recv()

    def spread(src, zz):
        for yy in y_others:
            tok_y(src, zz, yy).start()
        for cc in c_others:
            tok_c(src, zz, y, cc).start()

    def piece(kind, zz):
        if kind == 2:
            return d_ref.at[pl.ds(pl.multiple_of(zz * units, 128), units)]
        ref = g_ref if kind == 0 else v_ref
        return ref.at[:, pl.ds(pl.multiple_of(zz * units, 128), units)]

    def place(kind, src):
        if kind == 2:
            return dw.at[:, pl.ds(pl.multiple_of(src * cols, cols), cols)]
        ref = gw if kind == 0 else vw
        return ref.at[pl.ds(pl.multiple_of(src * depth, depth), depth)]

    def w_z(kind, zz):
        return copy(piece(kind, zz), place(kind, fs), wz_s.at[kind, zz], w_r.at[kind, fs], at(zz=zz))

    def w_x(kind, src, zz, xx):
        return copy(src, place(kind, zz * nx + x), wx_s.at[kind, zz, xx], w_r.at[kind, zz * nx + x], at(xx=xx))

    def w_wait(kind, src):
        copy(place(kind, src), place(kind, src), wz_s.at[kind, 0], w_r.at[kind, src], partners[0]).wait_recv()

    def w_own(kind):
        for xx in x_others:
            w_x(kind, piece(kind, z), z, xx).start()

    def w_send(kind):
        for zz in z_others:
            w_z(kind, zz).start()

    def w_forward(kind):
        for zz in z_others:
            w_wait(kind, zz * nx + x)
            for xx in x_others:
                w_x(kind, place(kind, zz * nx + x), zz, xx).start()

    def relay(step):
        for way in range(2):
            zz = z - step + 2 * step * way

            @pl.when((zz >= 0) & (zz < nz))
            def _():
                tok_wait(zz, tp)
                if step < nz - 1:
                    ahead = z + 1 - 2 * way

                    @pl.when((ahead >= 0) & (ahead < nz))
                    def _():
                        tok_z(slot(zz, tp), zz, way).start()
                spread(slot(zz, tp), zz)

    for way in range(2):
        ahead = z + 1 - 2 * way

        @pl.when((ahead >= 0) & (ahead < nz))
        def _():
            tok_z(x_ref, z, way).start()

    w_own(0)
    w_own(1)
    w_own(2)
    spread(x_ref, z)
    w_send(0)
    jobs = [lambda: w_send(1), lambda: w_forward(0), lambda: w_send(2), lambda: w_forward(1)]
    tok[z, pl.ds(pl.multiple_of(tp * rows, rows), rows)] = x_ref[...]
    mine = pl.ds(pl.multiple_of(fs * depth, depth), depth)
    part_units = pl.ds(pl.multiple_of(z * units, 128), units)
    gw[mine, :] = g_ref[:, part_units]
    vw[mine, :] = v_ref[:, part_units]
    dw[:, pl.ds(pl.multiple_of(fs * cols, cols), cols)] = d_ref[part_units, :]
    for step in range(1, nz):
        relay(step)
        for _ in range(2):
            if jobs:
                jobs.pop(0)()
    while jobs:
        jobs.pop(0)()
    for i in range(nz):
        zz = (z + i) % nz
        for yy in y_others:
            tok_wait(zz, yy * nc + c)
            for cc in c_others:
                tok_c(slot(zz, yy * nc + c), zz, yy, cc).start()
    w_forward(2)
    for kind in range(3):
        for xx in x_others:
            for i in range(nz):
                w_wait(kind, i * nx + xx)

    half = (2 * z) // nz if nz > 1 else 0
    near = z + half * (nz - 1 - 2 * z)

    def order(k):
        j = nz - 1 - k
        past = (j - near - 1 + nz) // nz
        f = past * j + (1 - past) * (near - j)
        return f + half * (nz - 1 - 2 * f)

    def block(zz, t):
        return part.at[zz, pl.ds(pl.multiple_of(t * rows, rows), rows)]

    def rc_copy(zz, yy, cc):
        return copy(block(zz, yy * nc + cc), rc.at[zz, yy], rc_s.at[zz, yy], rc_r.at[zz, yy], at(cc=cc))

    def ry_copy(zz, yy):
        return copy(block(zz, yy * nc + c), ry.at[zz, y], ry_s.at[zz, yy], ry_r.at[zz, y], at(yy=yy))

    def ry_wait(zz, yy):
        copy(block(zz, tp), ry.at[zz, yy], ry_s.at[zz, yy], ry_r.at[zz, yy], partners[0]).wait_recv()

    def zc_copy(way, zz):
        return copy(block(zz, tp), zr.at[way, zz], zc_s.at[way, zz], zc_r.at[way, zz], at(zz=z + 1 - 2 * way))

    def zc_wait(way, zz):
        copy(block(zz, tp), zr.at[way, zz], zc_s.at[way, zz], zc_r.at[way, zz], partners[0]).wait_recv()

    def mix(pre, w, taps, zz):
        raw = jnp.dot(tok[zz], w[...], preferred_element_type=jnp.float32)
        pre[pl.ds(LEAD, length), :] = raw.astype(jnp.bfloat16).astype(jnp.float32)
        return (
            taps[0:1, part_units] * pre[pl.ds(LEAD - 2, length), :]
            + taps[1:2, part_units] * pre[pl.ds(LEAD - 1, length), :]
            + taps[2:3, part_units] * pre[pl.ds(LEAD, length), :]
        )

    pre_g[0:LEAD, :] = jnp.zeros((LEAD, units), jnp.float32)
    pre_v[0:LEAD, :] = jnp.zeros((LEAD, units), jnp.float32)

    def f32(ref):
        return ref[...].astype(jnp.float32)

    def body(k, carry):
        @pl.when(k < nz)
        def _():
            zz = order(k)
            for yy in range(ny):
                for cc in c_others:
                    tok_wait(zz, yy * nc + cc)
            gate = mix(pre_g, gw, gt_ref, zz)
            value = mix(pre_v, vw, vt_ref, zz)
            act = 0.5 * gate * (1.0 + lax.erf(gate * (0.5**0.5)))
            hidden = (act * value).astype(jnp.bfloat16)
            part[zz] = jnp.dot(hidden, dw[...], preferred_element_type=jnp.float32).astype(jnp.bfloat16)
            for yy in range(ny):
                for cc in c_others:
                    rc_copy(zz, yy, cc).start()

        @pl.when((k >= 1) & (k < nz + 1))
        def _():
            zz = order(k - 1)
            for yy in y_others + [y]:
                if nc > 1:
                    rc_copy(zz, yy, c_others[0]).wait_recv()
                    mine = block(zz, yy * nc + c)
                    mine[...] = (f32(mine) + f32(rc.at[zz, yy])).astype(jnp.bfloat16)
            for yy in y_others:
                ry_copy(zz, yy).start()

        @pl.when(k >= 2)
        def _():
            zz = order(k - 2)
            mine = block(zz, tp)
            total = f32(mine)
            for yy in y_others:
                ry_wait(zz, yy)
                total = total + f32(ry.at[zz, yy])
            mine[...] = total.astype(jnp.bfloat16)
            t = k - 2
            for way in range(2):
                pos = z + way * (nz - 1 - 2 * z)
                far = nz - 1 - t + pos
                dest = far + way * (nz - 1 - 2 * far)

                @pl.when((t < nz - 1) & (t >= pos) & (pos < nz - 1))
                def _():
                    @pl.when(pos > 0)
                    def _():
                        zc_wait(way, dest)
                        sent = block(dest, tp)
                        sent[...] = (f32(sent) + f32(zr.at[way, dest])).astype(jnp.bfloat16)

                    zc_copy(way, dest).start()

        return carry

    lax.fori_loop(0, nz + 2, body, 0)

    for way in range(2):
        back = z - 1 + 2 * way

        @pl.when((back >= 0) & (back < nz))
        def _():
            zc_wait(way, z)

        @pl.when((back < 0) | (back >= nz))
        def _():
            zr[way, z] = jnp.zeros((rows, width), jnp.bfloat16)

    summed = f32(block(z, tp)) + f32(zr.at[0, z]) + f32(zr.at[1, z])
    average = jnp.mean(summed, axis=1, keepdims=True)
    centered = summed - average
    variance = jnp.mean(centered * centered, axis=1, keepdims=True)
    normed = centered * lax.rsqrt(variance + 1e-05) * gain_ref[...] + shift_ref[...]
    out_ref[...] = normed.astype(out_ref.dtype)

    for way in range(2):
        ahead = z + 1 - 2 * way

        @pl.when((ahead >= 0) & (ahead < nz))
        def _():
            for step in range(nz - 1):
                zz = z - step + 2 * step * way

                @pl.when((zz >= 0) & (zz < nz))
                def _():
                    tok_z(slot(zz, tp), zz, way).wait_send()

                dest = z + (step + 1) * (1 - 2 * way)

                @pl.when((dest >= 0) & (dest < nz))
                def _():
                    zc_copy(way, dest).wait_send()

    for zz in range(nz):
        for yy in y_others:
            tok_y(slot(zz, tp), zz, yy).wait_send()
            ry_copy(zz, yy).wait_send()
        for yy in range(ny):
            for cc in c_others:
                tok_c(slot(zz, yy * nc + c), zz, yy, cc).wait_send()
                rc_copy(zz, yy, cc).wait_send()
    for kind in range(3):
        for zz in z_others:
            w_z(kind, zz).wait_send()
        for zz in range(nz):
            for xx in x_others:
                w_x(kind, place(kind, zz * nx + x), zz, xx).wait_send()


def solution(mesh):
    n_fs, n_tp = mesh.shape["fs"], mesh.shape["tp"]
    nc = 2 if n_tp % 2 == 0 else 1
    ny = n_tp // nc

    def local(tokens, gate_weight, value_weight, gate_taps, value_taps, down_weight, gain, shift):
        rows, width = tokens.shape
        depth, held = gate_weight.shape
        nz = 4
        while nz > 1 and (n_fs % nz or held % (128 * nz)):
            nz //= 2
        nx = n_fs // nz
        units = held // nz
        length = n_tp * rows
        bf16 = jnp.bfloat16
        dma = pltpu.SemaphoreType.DMA
        return pl.pallas_call(
            functools.partial(kernel, (nz, nx, ny, nc)),
            out_shape=jax.ShapeDtypeStruct((rows, width), bf16),
            in_specs=[pl.BlockSpec(memory_space=pltpu.VMEM)] * 8,
            out_specs=pl.BlockSpec(memory_space=pltpu.VMEM),
            scratch_shapes=[
                pltpu.VMEM((nz, length, width), bf16),
                pltpu.VMEM((width, units), bf16),
                pltpu.VMEM((width, units), bf16),
                pltpu.VMEM((units, width), bf16),
                pltpu.VMEM((length + LEAD, units), jnp.float32),
                pltpu.VMEM((length + LEAD, units), jnp.float32),
                pltpu.VMEM((nz, length, width), bf16),
                pltpu.VMEM((nz, ny, rows, width), bf16),
                pltpu.VMEM((nz, ny, rows, width), bf16),
                pltpu.VMEM((2, nz, rows, width), bf16),
                dma((nz, n_tp)),
                dma((2, nz)),
                dma((nz, ny)),
                dma((nz, ny, nc)),
                dma((3, n_fs)),
                dma((3, nz)),
                dma((3, nz, nx)),
                dma((nz, ny)),
                dma((nz, ny)),
                dma((nz, ny)),
                dma((nz, ny)),
                dma((2, nz)),
                dma((2, nz)),
            ],
            compiler_params=pltpu.CompilerParams(
                collective_id=0, has_side_effects=True, vmem_limit_bytes=60 * 2**20
            ),
        )(
            tokens, gate_weight, value_weight, gate_taps, value_taps, down_weight,
            gain.reshape(1, width), shift.reshape(1, width),
        )

    in_specs = (
        P(("fs", "tp"), None),
        P("fs", "tp"),
        P("fs", "tp"),
        P(None, "tp"),
        P(None, "tp"),
        P("tp", "fs"),
        P(),
        P(),
    )
    out_specs = P(("fs", "tp"), None)
    return jax.shard_map(local, mesh=mesh, in_specs=in_specs, out_specs=out_specs, check_vma=False)
```

```python
import functools

import jax
import jax.numpy as jnp
from jax import lax
from jax.experimental import pallas as pl
from jax.experimental.pallas import tpu as pltpu
from jax.sharding import PartitionSpec as P

MESH = pl.DeviceIdType.MESH
LEAD = 8


def kernel(
    dims,
    x_ref, g_ref, v_ref, gt_ref, vt_ref, d_ref, gain_ref, shift_ref,
    out_ref,
    tok, gw, vw, dw, pre_g, pre_v, hid, part, rc, ry, zr,
    tok_r, tz_s, ty_s, tc_s, w_r, wz_s, wx_s, rc_r, rc_s, ry_r, ry_s, zc_r, zc_s,
):
    nz, nx, ny, nc = dims
    rows, width = x_ref.shape
    depth = g_ref.shape[0]
    units = gw.shape[1]
    cols = d_ref.shape[1]
    fs = lax.axis_index("fs")
    tp = lax.axis_index("tp")
    z, x = fs // nx, fs % nx
    y, c = tp // nc, tp % nc
    length = ny * nc * rows

    def at(zz=z, xx=x, yy=y, cc=c):
        return {"fs": zz * nx + xx, "tp": yy * nc + cc}

    z_others = [(z + i) % nz for i in range(1, nz)]
    x_others = [(x + i) % nx for i in range(1, nx)]
    y_others = [(y + i) % ny for i in range(1, ny)]
    c_others = [(c + i) % nc for i in range(1, nc)]

    barrier = pltpu.get_barrier_semaphore()
    partners = (
        [at(zz=i) for i in z_others]
        + [at(xx=i) for i in x_others]
        + [at(yy=i) for i in y_others]
        + [at(cc=i) for i in c_others]
    )
    for partner in partners:
        pl.semaphore_signal(barrier, inc=1, device_id=partner, device_id_type=MESH)
    pl.semaphore_wait(barrier, len(partners))

    def copy(src, dst, send, recv, device):
        return pltpu.make_async_remote_copy(
            src_ref=src, dst_ref=dst, send_sem=send, recv_sem=recv,
            device_id=device, device_id_type=MESH,
        )

    def slot(zz, t):
        return tok.at[zz, pl.ds(pl.multiple_of(t * rows, rows), rows)]

    def tok_copy(src, zz, t, send, device):
        return copy(src, slot(zz, t), send, tok_r.at[zz, t], device)

    def tok_z(src, zz, way):
        return tok_copy(src, zz, tp, tz_s.at[way, zz], at(zz=z + 1 - 2 * way))

    def tok_y(src, zz, yy):
        return tok_copy(src, zz, tp, ty_s.at[zz, yy], at(yy=yy))

    def tok_c(src, zz, yy, cc):
        return tok_copy(src, zz, yy * nc + c, tc_s.at[zz, yy, cc], at(cc=cc))

    def tok_wait(zz, t):
        tok_copy(slot(zz, t), zz, t, tz_s.at[0, 0], partners[0]).wait_recv()

    def spread(src, zz):
        for yy in y_others:
            tok_y(src, zz, yy).start()
        for cc in c_others:
            tok_c(src, zz, y, cc).start()

    def piece(kind, zz):
        if kind == 2:
            return d_ref.at[pl.ds(pl.multiple_of(zz * units, 128), units)]
        ref = g_ref if kind == 0 else v_ref
        return ref.at[:, pl.ds(pl.multiple_of(zz * units, 128), units)]

    def place(kind, src):
        if kind == 2:
            return dw.at[:, pl.ds(pl.multiple_of(src * cols, cols), cols)]
        ref = gw if kind == 0 else vw
        return ref.at[pl.ds(pl.multiple_of(src * depth, depth), depth)]

    def w_z(kind, zz):
        return copy(piece(kind, zz), place(kind, fs), wz_s.at[kind, zz], w_r.at[kind, fs], at(zz=zz))

    def w_x(kind, src, zz, xx):
        return copy(src, place(kind, zz * nx + x), wx_s.at[kind, zz, xx], w_r.at[kind, zz * nx + x], at(xx=xx))

    def w_wait(kind, src):
        copy(place(kind, src), place(kind, src), wz_s.at[kind, 0], w_r.at[kind, src], partners[0]).wait_recv()

    def w_own(kind):
        for xx in x_others:
            w_x(kind, piece(kind, z), z, xx).start()

    def both(step, act):
        for way in range(2):
            zz = z - step + 2 * step * way

            @pl.when((zz >= 0) & (zz < nz))
            def _():
                act(zz)

    def w_send(kind):
        for step in range(1, nz):
            both(step, lambda zz: w_z(kind, zz).start())

    def w_forward(kind, step):
        def act(zz):
            w_wait(kind, zz * nx + x)
            for xx in x_others:
                w_x(kind, place(kind, zz * nx + x), zz, xx).start()

        both(step, act)

    def relay(step):
        for way in range(2):
            zz = z - step + 2 * step * way

            @pl.when((zz >= 0) & (zz < nz))
            def _():
                tok_wait(zz, tp)
                if step < nz - 1:
                    ahead = z + 1 - 2 * way

                    @pl.when((ahead >= 0) & (ahead < nz))
                    def _():
                        tok_z(slot(zz, tp), zz, way).start()
                spread(slot(zz, tp), zz)

    for way in range(2):
        ahead = z + 1 - 2 * way

        @pl.when((ahead >= 0) & (ahead < nz))
        def _():
            tok_z(x_ref, z, way).start()

    w_own(0)
    spread(x_ref, z)
    w_own(1)
    tok[z, pl.ds(pl.multiple_of(tp * rows, rows), rows)] = x_ref[...]
    mine = pl.ds(pl.multiple_of(fs * depth, depth), depth)
    part_units = pl.ds(pl.multiple_of(z * units, 128), units)
    gw[mine, :] = g_ref[:, part_units]
    vw[mine, :] = v_ref[:, part_units]
    dw[:, pl.ds(pl.multiple_of(fs * cols, cols), cols)] = d_ref[part_units, :]
    for step in range(1, nz):
        relay(step)
        if step == min(2, nz - 1):
            for kind in range(3):
                w_send(kind)
            w_own(2)
    for kind in range(2):
        for step in range(1, nz):
            w_forward(kind, step)

    half = (2 * z) // nz if nz > 1 else 0
    near = z + half * (nz - 1 - 2 * z)

    def order(j):
        past = (j - near - 1 + nz) // nz
        f = past * j + (1 - past) * (near - j)
        return f + half * (nz - 1 - 2 * f)

    def far_order(k):
        return order(nz - 1 - k)

    def cross(zz):
        for yy in y_others:
            tok_wait(zz, yy * nc + c)
            for cc in c_others:
                tok_c(slot(zz, yy * nc + c), zz, yy, cc).start()

    cross(order(0))
    for kind in range(2):
        for xx in x_others:
            for i in range(nz):
                w_wait(kind, i * nx + xx)

    def block(zz, t):
        return part.at[zz, pl.ds(pl.multiple_of(t * rows, rows), rows)]

    def rc_copy(zz, yy, cc):
        return copy(block(zz, yy * nc + cc), rc.at[zz, yy], rc_s.at[zz, yy], rc_r.at[zz, yy], at(cc=cc))

    def ry_copy(zz, yy):
        return copy(block(zz, yy * nc + c), ry.at[zz, y], ry_s.at[zz, yy], ry_r.at[zz, y], at(yy=yy))

    def ry_wait(zz, yy):
        copy(block(zz, tp), ry.at[zz, yy], ry_s.at[zz, yy], ry_r.at[zz, yy], partners[0]).wait_recv()

    def zc_copy(way, zz):
        return copy(block(zz, tp), zr.at[way, zz], zc_s.at[way, zz], zc_r.at[way, zz], at(zz=z + 1 - 2 * way))

    def zc_wait(way, zz):
        copy(block(zz, tp), zr.at[way, zz], zc_s.at[way, zz], zc_r.at[way, zz], partners[0]).wait_recv()

    def mix(pre, w, taps, zz):
        raw = jnp.dot(tok[zz], w[...], preferred_element_type=jnp.float32)
        pre[pl.ds(LEAD, length), :] = raw.astype(jnp.bfloat16).astype(jnp.float32)
        return (
            taps[0:1, part_units] * pre[pl.ds(LEAD - 2, length), :]
            + taps[1:2, part_units] * pre[pl.ds(LEAD - 1, length), :]
            + taps[2:3, part_units] * pre[pl.ds(LEAD, length), :]
        )

    pre_g[0:LEAD, :] = jnp.zeros((LEAD, units), jnp.float32)
    pre_v[0:LEAD, :] = jnp.zeros((LEAD, units), jnp.float32)

    def f32(ref):
        return ref[...].astype(jnp.float32)

    for k in range(nz):
        zz = order(k)
        if k + 1 < nz:
            cross(order(k + 1))
        for yy in range(ny):
            for cc in c_others:
                tok_wait(zz, yy * nc + cc)
        gate = mix(pre_g, gw, gt_ref, zz)
        value = mix(pre_v, vw, vt_ref, zz)
        act = 0.5 * gate * (1.0 + lax.erf(gate * (0.5**0.5)))
        hid[zz] = (act * value).astype(jnp.bfloat16)
        if k + 1 < nz:
            w_forward(2, k + 1)
    for xx in x_others:
        for i in range(nz):
            w_wait(2, i * nx + xx)

    def body(k, carry):
        @pl.when(k < nz)
        def _():
            zz = far_order(k)
            part[zz] = jnp.dot(hid[zz], dw[...], preferred_element_type=jnp.float32).astype(jnp.bfloat16)
            for yy in range(ny):
                for cc in c_others:
                    rc_copy(zz, yy, cc).start()

        @pl.when((k >= 1) & (k < nz + 1))
        def _():
            zz = far_order(k - 1)
            for yy in y_others + [y]:
                if nc > 1:
                    rc_copy(zz, yy, c_others[0]).wait_recv()
                    mine = block(zz, yy * nc + c)
                    mine[...] = (f32(mine) + f32(rc.at[zz, yy])).astype(jnp.bfloat16)
            for yy in y_others:
                ry_copy(zz, yy).start()

        @pl.when(k >= 2)
        def _():
            zz = far_order(k - 2)
            mine = block(zz, tp)
            total = f32(mine)
            for yy in y_others:
                ry_wait(zz, yy)
                total = total + f32(ry.at[zz, yy])
            mine[...] = total.astype(jnp.bfloat16)
            t = k - 2
            for way in range(2):
                pos = z + way * (nz - 1 - 2 * z)
                far = nz - 1 - t + pos
                dest = far + way * (nz - 1 - 2 * far)

                @pl.when((t < nz - 1) & (t >= pos) & (pos < nz - 1))
                def _():
                    @pl.when(pos > 0)
                    def _():
                        zc_wait(way, dest)
                        sent = block(dest, tp)
                        sent[...] = (f32(sent) + f32(zr.at[way, dest])).astype(jnp.bfloat16)

                    zc_copy(way, dest).start()

        return carry

    lax.fori_loop(0, nz + 2, body, 0)

    for way in range(2):
        back = z - 1 + 2 * way

        @pl.when((back >= 0) & (back < nz))
        def _():
            zc_wait(way, z)

        @pl.when((back < 0) | (back >= nz))
        def _():
            zr[way, z] = jnp.zeros((rows, width), jnp.bfloat16)

    summed = f32(block(z, tp)) + f32(zr.at[0, z]) + f32(zr.at[1, z])
    average = jnp.mean(summed, axis=1, keepdims=True)
    centered = summed - average
    variance = jnp.mean(centered * centered, axis=1, keepdims=True)
    normed = centered * lax.rsqrt(variance + 1e-05) * gain_ref[...] + shift_ref[...]
    out_ref[...] = normed.astype(out_ref.dtype)

    for way in range(2):
        ahead = z + 1 - 2 * way

        @pl.when((ahead >= 0) & (ahead < nz))
        def _():
            for step in range(nz - 1):
                zz = z - step + 2 * step * way

                @pl.when((zz >= 0) & (zz < nz))
                def _():
                    tok_z(slot(zz, tp), zz, way).wait_send()

                dest = z + (step + 1) * (1 - 2 * way)

                @pl.when((dest >= 0) & (dest < nz))
                def _():
                    zc_copy(way, dest).wait_send()

    for zz in range(nz):
        for yy in y_others:
            tok_y(slot(zz, tp), zz, yy).wait_send()
            ry_copy(zz, yy).wait_send()
        for yy in range(ny):
            for cc in c_others:
                tok_c(slot(zz, yy * nc + c), zz, yy, cc).wait_send()
                rc_copy(zz, yy, cc).wait_send()
    for kind in range(3):
        for zz in z_others:
            w_z(kind, zz).wait_send()
        for zz in range(nz):
            for xx in x_others:
                w_x(kind, place(kind, zz * nx + x), zz, xx).wait_send()


def solution(mesh):
    n_fs, n_tp = mesh.shape["fs"], mesh.shape["tp"]
    nc = 2 if n_tp % 2 == 0 else 1
    ny = n_tp // nc

    def local(tokens, gate_weight, value_weight, gate_taps, value_taps, down_weight, gain, shift):
        rows, width = tokens.shape
        depth, held = gate_weight.shape
        nz = 4
        while nz > 1 and (n_fs % nz or held % (128 * nz)):
            nz //= 2
        nx = n_fs // nz
        units = held // nz
        length = n_tp * rows
        bf16 = jnp.bfloat16
        dma = pltpu.SemaphoreType.DMA
        return pl.pallas_call(
            functools.partial(kernel, (nz, nx, ny, nc)),
            out_shape=jax.ShapeDtypeStruct((rows, width), bf16),
            in_specs=[pl.BlockSpec(memory_space=pltpu.VMEM)] * 8,
            out_specs=pl.BlockSpec(memory_space=pltpu.VMEM),
            scratch_shapes=[
                pltpu.VMEM((nz, length, width), bf16),
                pltpu.VMEM((width, units), bf16),
                pltpu.VMEM((width, units), bf16),
                pltpu.VMEM((units, width), bf16),
                pltpu.VMEM((length + LEAD, units), jnp.float32),
                pltpu.VMEM((length + LEAD, units), jnp.float32),
                pltpu.VMEM((nz, length, units), bf16),
                pltpu.VMEM((nz, length, width), bf16),
                pltpu.VMEM((nz, ny, rows, width), bf16),
                pltpu.VMEM((nz, ny, rows, width), bf16),
                pltpu.VMEM((2, nz, rows, width), bf16),
                dma((nz, n_tp)),
                dma((2, nz)),
                dma((nz, ny)),
                dma((nz, ny, nc)),
                dma((3, n_fs)),
                dma((3, nz)),
                dma((3, nz, nx)),
                dma((nz, ny)),
                dma((nz, ny)),
                dma((nz, ny)),
                dma((nz, ny)),
                dma((2, nz)),
                dma((2, nz)),
            ],
            compiler_params=pltpu.CompilerParams(
                collective_id=0, has_side_effects=True, vmem_limit_bytes=60 * 2**20
            ),
        )(
            tokens, gate_weight, value_weight, gate_taps, value_taps, down_weight,
            gain.reshape(1, width), shift.reshape(1, width),
        )

    in_specs = (
        P(("fs", "tp"), None),
        P("fs", "tp"),
        P("fs", "tp"),
        P(None, "tp"),
        P(None, "tp"),
        P("tp", "fs"),
        P(),
        P(),
    )
    out_specs = P(("fs", "tp"), None)
    return jax.shard_map(local, mesh=mesh, in_specs=in_specs, out_specs=out_specs, check_vma=False)
```
